32 devices in a mesh: ep: 8 (over z, y), tp: 4 (over x, core).
Axes of the slice: x: 2, y: 2, z: 4, core: 2. Of those that a mesh axis runs over, the one named last changes fastest.
Arguments:
- query: bfloat16 [8192, 1024], P('ep', 'tp'), may hold values from -6 to 6
- keys: bfloat16 [8192, 1024], P('ep', 'tp'), may hold values from -6 to 6
- values: bfloat16 [8192, 2048], P('ep', 'tp'), may hold values from -6 to 6
- gate_pre: bfloat16 [8192, 2048], P('ep', 'tp'), may hold values from -6 to 6
- log_decay: float32 [16, 8192], P('tp', 'ep'), may hold values from -1 to 0
- out_weight: bfloat16 [2048, 4096], P(None, 'tp'), may hold values from -0.125 to 0.125
- expert_input: bfloat16 [2048, 4096], P(('ep', 'tp')), may hold values from -6 to 6
- norm_gain: float32 [4096], replicated, may hold values from 0.1 to 1.9
- routes: int32 [2048, 2], P(('ep', 'tp')), may hold values from 0 to 7, all different within a row; in each aligned block of 64 rows (0 to 63, 64 to 127, ...) at most 24 rows name the same one
- route_weights: float32 [2048, 2], P(('ep', 'tp')), may hold values from 0.1 to 1
- w_gate: bfloat16 [8, 4096, 1536], P('ep', None, 'tp'), may hold values from -0.09375 to 0.09375
- w_up: bfloat16 [8, 4096, 1536], P('ep', None, 'tp'), may hold values from -0.09375 to 0.09375
- w_down: bfloat16 [8, 1536, 4096], P('ep', 'tp'), may hold values from -0.15625 to 0.15625
Outputs:
- mixed: bfloat16 [8192, 4096], P('ep', 'tp')
- moe_out: bfloat16 [2048, 4096], P(('ep', 'tp'))
The draws below stay inside these ranges and needn't reach their ends.
Inputs may be any that keep to these rules, and one draw needn't show every extreme that they name: `routes`: each row names 2 different experts; among the rows of one device no expert is named by more than 24 rows, a bound that some block reaches of some device.
All inputs are finite; a program needn't handle non-finite values.
Results may differ from the reference program's by a relative error of at most 0.018.
Values may be sent and summed in bfloat16 or wider, within the bound.
A program may use at most 128 MiB of HBM per device.

```python
import math
import jax
import jax.numpy as jnp
import numpy as np
from jax import lax

D = 4096
RETENTION_HEADS = 16
DK = 64
DV = 128
FFE = 1536
TOP = 2
BLK = 128
TB_DEV = 64
EXPERTS = 8
CAP = 24
ROWS_A = 1024
FIRST_TOKENS = 8192
TOKENS_B = 2048
N_EP = 8
N_TP = 4


def draw_log_decay(key, part):
    key_sequence = jax.random.split(jax.random.fold_in(key, 71), 7)
    fast_share = 0.5
    fast_heads = jax.random.uniform(key_sequence[0], (RETENTION_HEADS,), jnp.float32) < fast_share
    fast_rate = jnp.exp(jax.random.uniform(key_sequence[1], (RETENTION_HEADS,), jnp.float32, jnp.log(1.0 / 80.0), jnp.log(1.0 / 30.0)))
    slow_rate = jax.random.uniform(key_sequence[2], (RETENTION_HEADS,), jnp.float32, 0.3, 0.8) / FIRST_TOKENS
    base_rate = jnp.where(fast_heads, fast_rate, slow_rate)
    span_len = max(ROWS_A // 2, 1)
    span_count = FIRST_TOKENS // span_len
    span_factor = jnp.exp(jax.random.uniform(key_sequence[3], (RETENTION_HEADS, span_count), jnp.float32, jnp.log(0.4), jnp.log(2.5)))
    span_factor = jnp.repeat(span_factor, span_len, axis=1)
    roughness = jnp.exp(jax.random.uniform(key_sequence[4], (RETENTION_HEADS, FIRST_TOKENS), jnp.float32, -0.5, 0.5))
    logarithm_rate = -(base_rate[:, None] * span_factor * roughness)
    spike_position = jax.random.randint(key_sequence[5], (3,), 0, FIRST_TOKENS)
    spike_strength = jnp.log(jax.random.uniform(key_sequence[6], (RETENTION_HEADS, 3), jnp.float32, 0.5, 0.8))
    position_index = jnp.arange(FIRST_TOKENS, dtype=jnp.int32)
    expert_hits = (position_index[None, :] == spike_position[:, None]).astype(jnp.float32)
    decay_spikes = jnp.dot(spike_strength, expert_hits)
    return (logarithm_rate + decay_spikes).astype(jnp.float32)


def steps_of(key, extent, cuts, low, high):
    gain, own = 1.0, jax.random.fold_in(key, 6)
    for axis_at, blocks in cuts:
        steps = jnp.exp(jax.random.uniform(jax.random.fold_in(own, axis_at), (blocks,), jnp.float32, low / len(cuts), high / len(cuts)))
        gain = gain * jnp.repeat(steps, extent[axis_at] // blocks).reshape([-1 if axis == axis_at else 1 for axis in range(len(extent))])
    return gain


def deal_out(stream_key, own, number, rows, count, top, most, slope):
    order = jax.random.permutation(stream_key, count)
    crowded, common = portions_of(count, rows * top, most, slope, True), portions_of(count, rows * top, most, slope, False)
    places = jnp.arange(count)

    def named(tallies, offset_by):
        used = int((tallies > 0).sum())
        fixed = max(1, used // 4)
        passed = fixed + (places - fixed + offset_by * (used - fixed)) % max(1, count - fixed)
        return jnp.zeros((count,), jnp.int32).at[order[jnp.where(places < fixed, places, passed)]].set(jnp.asarray(tallies, jnp.int32))

    tallies = jnp.where(number % 4 == 0, named(crowded, number // 4), named(common, number - number // 4 - 1))
    mixed = jax.random.permutation(jax.random.fold_in(own, 3), count)
    donor, sink = mixed[0:count // 2 * 2:2], mixed[1:count // 2 * 2:2]
    slack = jnp.minimum(tallies[donor] - 1, most - tallies[sink]) // 2
    slack = jnp.where((donor == order[0]) | (sink == order[0]) | (tallies[sink] == 0), 0, jnp.maximum(slack, 0))
    passed = jax.random.randint(jax.random.fold_in(own, 4), (count // 2,), 0, 1 << 20) % (slack + 1)
    tallies = tallies.at[donor].add(-passed).at[sink].add(passed)
    items = jnp.searchsorted(jnp.cumsum(tallies), jnp.arange(rows * top), side="right").astype(jnp.int32)
    listing = items.reshape(top, rows).T
    listing = listing[jax.random.permutation(jax.random.fold_in(own, 1), rows)]
    offset_by = jax.random.randint(jax.random.fold_in(own, 2), (rows, 1), 0, top)
    return jnp.take_along_axis(listing, (jnp.arange(top)[None, :] + offset_by) % top, axis=1)


def portions_of(number_of, total, bound, lean, full):
    weights = [(1 << 20) // math.isqrt(rank ** lean) + 1 for rank in range(1, number_of + 1)]
    largest = bound if full else min(bound, max(-(-total // number_of), total * weights[0] // sum(weights)))
    least = 1 if total - largest >= number_of - 1 else 0
    given, surplus = [largest] + [least] * (number_of - 1), total - largest - least * (number_of - 1)
    while surplus > 0:
        candidates = [i for i in range(1, number_of) if given[i] < largest] or [i for i in range(1, number_of) if given[i] < bound]
        whole, left = sum([weights[i] for i in candidates]), surplus
        for i in candidates:
            more = min(bound - given[i], max(1, left * weights[i] // whole), surplus)
            given[i] = given[i] + more
            surplus = surplus - more
    return np.array(given)


def noise(rng, shape, deviation, reach, cuts=(), kind=jnp.bfloat16):
    factor_of = steps_of(rng, shape, cuts, -0.22, 0.18) if cuts else 1.0
    values = jax.random.normal(rng, shape, jnp.float32) * deviation * factor_of
    return jnp.minimum(jnp.maximum(values, -reach), reach).astype(kind)


def setup_inputs(seed: int = 0) -> dict:
    arg_keys = jax.random.split(jax.random.key(seed), 14)
    query = noise(arg_keys[0], (FIRST_TOKENS, RETENTION_HEADS * DK), 1.0, 6.0, ((0, 8), (1, 4)))
    keys = noise(arg_keys[1], (FIRST_TOKENS, RETENTION_HEADS * DK), 1.0, 6.0, ((0, 8), (1, 4)))
    values = noise(arg_keys[2], (FIRST_TOKENS, RETENTION_HEADS * DV), 1.0, 6.0, ((0, 8), (1, 4)))
    gate_pre = noise(arg_keys[3], (FIRST_TOKENS, RETENTION_HEADS * DV), 1.0, 6.0, ((0, 8), (1, 4)))
    log_decay = draw_log_decay(jax.random.fold_in(arg_keys[13], 71), 0)
    out_weight = noise(arg_keys[5], (RETENTION_HEADS * DV, D), (RETENTION_HEADS * DV) ** -0.5, 0.125, ((1, 4),))
    expert_input = noise(arg_keys[6], (TOKENS_B, D), 1.0, 6.0, ((0, 32),))
    norm_gain = jnp.clip(1.0 + 0.18 * jax.random.normal(arg_keys[7], (D,), jnp.float32), 0.1, 1.9)
    routes_keys = jax.random.split(jax.random.fold_in(arg_keys[8], 1), TOKENS_B // TB_DEV)
    routes_turns = jax.random.permutation(jax.random.fold_in(arg_keys[8], 3), TOKENS_B // TB_DEV)
    routes = jax.vmap(lambda own, number: deal_out(jax.random.fold_in(arg_keys[8], 2), own, number, TB_DEV, EXPERTS, TOP, CAP, 1))(routes_keys, routes_turns).reshape((TOKENS_B, TOP))
    route_weights = jnp.clip(0.1 + 0.9 * jax.random.uniform(arg_keys[9], (TOKENS_B, TOP), jnp.float32) ** steps_of(arg_keys[9], (TOKENS_B, TOP), ((0, 32),), -0.2, 0.2), 0.1, 1.0)
    w_gate = noise(arg_keys[10], (EXPERTS, D, FFE), D ** -0.5, 0.09375, ((0, 8), (2, 4)))
    w_up = noise(arg_keys[11], (EXPERTS, D, FFE), D ** -0.5, 0.09375, ((0, 8), (2, 4)))
    w_down = noise(arg_keys[12], (EXPERTS, FFE, D), FFE ** -0.5, 0.15625, ((0, 8), (1, 4)))
    return {"query": query, "keys": keys, "values": values, "gate_pre": gate_pre, "log_decay": log_decay, "out_weight": out_weight, "expert_input": expert_input, "norm_gain": norm_gain, "routes": routes, "route_weights": route_weights, "w_gate": w_gate, "w_up": w_up, "w_down": w_down}


def rotate(vectors, position_index):
    half_dim = vectors.shape[-1] // 2
    inverse = 1.0 / 10000.0 ** jnp.linspace(0.0, 1.0, half_dim, dtype=jnp.float32)
    angles = position_index[:, None] * inverse[None, :]
    cosine = jnp.cos(angles)[:, None, :]
    sine_part = jnp.sin(angles)[:, None, :]
    first_half = vectors[..., :half_dim]
    second_half = vectors[..., half_dim:]
    return jnp.concatenate([first_half * cosine - second_half * sine_part, first_half * sine_part + second_half * cosine], axis=-1)

def retention_block(state, inputs):
    query_blk, key_blk, value_blk, decay_blk = inputs
    width_blk = decay_blk.shape[1]
    running = jnp.cumsum(decay_blk, axis=1)
    spread = running[:, :, None] - running[:, None, :]
    causal = jnp.tril(jnp.ones((width_blk, width_blk), dtype=bool))[None]
    weights = jnp.where(causal, jnp.exp(jnp.where(causal, spread, 0.0)), 0.0)
    highest = lax.Precision.HIGHEST
    scores = jnp.einsum('hid,hjd->hij', query_blk, key_blk, precision=highest) * weights
    output = jnp.einsum('hij,hje->hie', scores, value_blk, precision=highest)
    output = output + jnp.einsum('hid,hde->hie', query_blk * jnp.exp(running)[:, :, None], state, precision=highest)
    closing = running[:, -1:]
    state_next = state * jnp.exp(closing)[:, :, None] + jnp.einsum('hjd,hje->hde', key_blk * jnp.exp(closing - running)[:, :, None], value_blk, precision=highest)
    return (state_next, output)

def head_norm(vectors):
    centered = vectors - lax.optimization_barrier(jnp.mean(vectors, axis=-1, keepdims=True))
    variance = lax.optimization_barrier(jnp.mean(centered * centered, axis=-1, keepdims=True))
    return centered * lax.rsqrt(variance + 1e-06)

def mixer(query, keys, values, gate_pre, log_decay, out_weight):
    length = query.shape[0]
    position_index = jnp.arange(length, dtype=jnp.int32).astype(jnp.float32)
    rotated_q = rotate(query.astype(jnp.float32).reshape(length, RETENTION_HEADS, DK), position_index)
    rotated_k = rotate(keys.astype(jnp.float32).reshape(length, RETENTION_HEADS, DK), position_index) * DK ** (-0.5)
    value_rows = values.astype(jnp.float32).reshape(length, RETENTION_HEADS, DV)
    block_count = length // BLK

    def to_blocks(array):
        return array.reshape(block_count, BLK, RETENTION_HEADS, array.shape[-1]).transpose(0, 2, 1, 3)
    decay_blocks = log_decay.reshape(RETENTION_HEADS, block_count, BLK).transpose(1, 0, 2)
    start_state = jnp.zeros((RETENTION_HEADS, DK, DV), jnp.float32)
    final_state, outputs = lax.scan(retention_block, start_state, (to_blocks(rotated_q), to_blocks(rotated_k), to_blocks(value_rows), decay_blocks))
    combined = outputs.transpose(0, 2, 1, 3).reshape(length, RETENTION_HEADS, DV)
    gate_act = jax.nn.silu(gate_pre.astype(jnp.float32).reshape(length, RETENTION_HEADS, DV))
    gated = (gate_act * head_norm(combined)).reshape(length, RETENTION_HEADS * DV).astype(jnp.bfloat16)
    return jnp.dot(gated, out_weight, preferred_element_type=jnp.float32).astype(jnp.bfloat16)

def experts(expert_input, norm_gain, routes, route_weights, w_gate, w_up, w_down):
    rows_f = expert_input.astype(jnp.float32)
    centered = rows_f - lax.optimization_barrier(jnp.mean(rows_f, axis=-1, keepdims=True))
    variance = lax.optimization_barrier(jnp.mean(centered * centered, axis=-1, keepdims=True))
    normed = (centered * lax.rsqrt(variance + 1e-05) * norm_gain).astype(jnp.bfloat16)
    pair_count = TOKENS_B * TOP
    expert_ids = routes.reshape(pair_count).astype(jnp.int32)
    limit = N_EP * N_TP * CAP
    block_width = FFE // N_TP

    def one_expert(pair_out, index):
        chosen = jnp.nonzero(expert_ids == index, size=limit, fill_value=pair_count)[0].astype(jnp.int32)
        token_rows = jnp.minimum(chosen // TOP, TOKENS_B - 1).astype(jnp.int32)
        rows_in = normed[token_rows]
        gate_w = lax.dynamic_index_in_dim(w_gate, index, 0, keepdims=False)
        up_w = lax.dynamic_index_in_dim(w_up, index, 0, keepdims=False)
        down_w = lax.dynamic_index_in_dim(w_down, index, 0, keepdims=False)
        hidden = (jax.nn.silu(jnp.dot(rows_in, gate_w, preferred_element_type=jnp.float32)) * jnp.dot(rows_in, up_w, preferred_element_type=jnp.float32)).astype(jnp.bfloat16)
        total = jnp.zeros((limit, D), jnp.float32)
        for part_index in range(N_TP):
            lower = part_index * block_width
            part_rows = jnp.dot(hidden[:, lower:lower + block_width], down_w[lower:lower + block_width], preferred_element_type=jnp.float32).astype(jnp.bfloat16)
            total = total + lax.optimization_barrier(part_rows).astype(jnp.float32)
        pair_out = pair_out.at[chosen].set(total.astype(jnp.bfloat16), mode='drop')
        return (pair_out, None)
    pair_out, _ = lax.scan(one_expert, jnp.zeros((pair_count, D), jnp.bfloat16), jnp.arange(EXPERTS, dtype=jnp.int32))
    weighted = pair_out.reshape(TOKENS_B, TOP, D).astype(jnp.float32) * route_weights[:, :, None]
    return lax.optimization_barrier(jnp.sum(weighted, axis=1)).astype(jnp.bfloat16)

def reference(query, keys, values, gate_pre, log_decay, out_weight, expert_input, norm_gain, routes, route_weights, w_gate, w_up, w_down):
    mixed = mixer(query, keys, values, gate_pre, log_decay, out_weight)
    moe_out = experts(expert_input, norm_gain, routes, route_weights, w_gate, w_up, w_down)
    return (mixed, moe_out)
```

```python
import functools
import jax
import jax.numpy as jnp
import numpy as np
from jax import lax
from jax.experimental import pallas as pl
from jax.experimental.pallas import tpu as pltpu
from jax.sharding import PartitionSpec as P

BF = jnp.bfloat16
F32 = jnp.float32
VM = pltpu.VMEM
ANY = pl.ANY
MESH = pl.DeviceIdType.MESH
DMA = pltpu.SemaphoreType.DMA
BLOCK = 256
COLS = 512


def flip(index, bits):
    out = index
    bit = 1
    while bit <= bits:
        if bits & bit:
            out = out + bit - 2 * bit * lax.rem(lax.div(index, bit), 2)
        bit *= 2
    return out


def dot(a, b):
    return jnp.dot(a, b, preferred_element_type=F32)


def turn(x, cos, sin, head_dim):
    width = x.shape[1]
    half = head_dim // 2
    lane = lax.broadcasted_iota(jnp.int32, x.shape, 1)
    first = lane % head_dim < half
    other = jnp.where(first, pltpu.roll(x, width - half, 1), pltpu.roll(x, half, 1))
    reps = width // cos.shape[1]
    return x * jnp.concatenate([cos] * reps, axis=1) + other * jnp.concatenate([sin] * reps, axis=1)


class Sizes:
    def __init__(self, ep, tokens, width, top, rows, heads, dk, dv, hidden, features):
        self.ep, self.tokens, self.width, self.top = ep, tokens, width, top
        self.rows, self.heads, self.dk, self.dv = rows, heads, dk, dv
        self.hidden, self.features = hidden, features
        self.half = width // 2
        self.cap = 3 * tokens * top // (2 * ep)
        self.one = -(-2 * self.cap // 16) * 16
        self.two = 2 * self.one
        self.near = ep // 2
        self.blocks = rows // BLOCK
        self.stages = ep.bit_length() - 1


def kernel(
    z,
    q_hbm, k_hbm, v_hbm, g_hbm, decay_ref, wo_hbm, tok_hbm, gain_ref, routes_ref, rweight_ref,
    wg_hbm, wu_hbm, wd_hbm, spin_ref, base_ref,
    mixed_hbm, moe_hbm,
    q_v, k_v, v_v, g_v, wo_v, tok_v, wg_v, wu_v, wd_v,
    nh, nb, meta, sn, sc, xf, yk, ys, yr, xr, zc, rn, rc, own, fxs, fxr, fin,
    wnh, wnl, wch, wcl, pn, keyt, upd, run_v, runt_v, pack_s, pack_r, pre_v, gate_all, mix_v,
    load_sem, send_sem, recv_sem, out_sem,
):
    e = lax.axis_index("ep")
    t = lax.axis_index("tp")
    c = lax.rem(t, 2)
    o = 1 - c
    pair = (e, flip(t, 1))
    cross = (e, flip(t, 2))
    diag = (e, flip(t, 3))
    H, ONE, TWO, NEAR, TOK, CAP = z.half, z.one, z.two, z.near, z.tokens, z.cap
    used = [0]
    sent = []

    barrier = pltpu.get_barrier_semaphore()
    peers = [(flip(e, d), t) for d in range(1, z.ep)] + [pair, cross, diag]
    for peer in peers:
        pl.semaphore_signal(barrier, inc=1, device_id=peer, device_id_type=MESH)

    loads = {}

    def load(name, src, dst):
        copy = pltpu.make_async_copy(src, dst, load_sem.at[len(loads)])
        copy.start()
        loads[name] = copy

    load("tok", tok_hbm, tok_v)
    load("k", k_hbm, k_v)
    load("v", v_hbm, v_v)
    load("q", q_hbm, q_v)
    load("g", g_hbm, g_v)
    load("wg", wg_hbm.at[0], wg_v)
    load("wu", wu_hbm.at[0], wu_v)
    for h in range(2):
        load("wd%d" % h, wd_hbm.at[0, :, pl.ds(h * H, H)], wd_v.at[h])
    load("wo", wo_hbm, wo_v)

    def send(src, dst, device):
        i = used[0]
        used[0] += 1
        copy = pltpu.make_async_remote_copy(
            src_ref=src, dst_ref=dst, send_sem=send_sem.at[i], recv_sem=recv_sem.at[i],
            device_id=device, device_id_type=MESH,
        )
        copy.start()
        sent.append(copy)
        return copy

    lane = lax.broadcasted_iota(jnp.int32, (TOK, 128), 1)
    packed = jnp.zeros((TOK, 128), F32)
    for r in range(2):
        packed = packed + jnp.where(lane == r, routes_ref[:, r : r + 1].astype(F32), 0.0)
        packed = packed + jnp.where(lane == 2 + r, rweight_ref[:, r : r + 1], 0.0)
    meta[c] = packed
    pl.semaphore_wait(barrier, len(peers))
    metas = [
        send(meta.at[c], meta.at[c], pair),
        send(meta.at[c], meta.at[2 + c], cross),
        send(meta.at[c], meta.at[2 + c], diag),
    ]

    loads["tok"].wait()
    x = tok_v[...].astype(F32)
    centered = x - jnp.mean(x, axis=-1, keepdims=True)
    variance = jnp.mean(centered * centered, axis=-1, keepdims=True)
    normed = (centered * lax.rsqrt(variance + 1e-05) * gain_ref[...]).astype(BF)
    nh[0] = normed[:, :H]
    nh[1] = normed[:, H:]
    toks = [
        send(nh.at[o], nb.at[c], pair),
        send(nh.at[c], nb.at[2 + c], cross),
        send(nh.at[o], nb.at[2 + c], diag),
    ]
    nb[c] = nh[c]

    for copy in metas:
        copy.wait_recv()
    every = 4 * TOK
    info = meta[...].reshape(every, 128)
    number = lax.broadcasted_iota(jnp.int32, (every, 128), 1)
    token = lax.broadcasted_iota(jnp.int32, (every, 1), 0)
    away = lax.div(token, 2 * TOK)
    side = lax.rem(lax.div(token, TOK), 2)
    rel = [jnp.bitwise_xor(info[:, r : r + 1].astype(jnp.int32), e) for r in range(2)]
    hits = [(rel[r] == number).astype(F32) for r in range(2)]
    i = lax.broadcasted_iota(jnp.int32, (every, every), 0)
    j = lax.broadcasted_iota(jnp.int32, (every, every), 1)
    earlier = ((j < i) & (lax.div(i, TOK) == lax.div(j, TOK))).astype(F32).astype(BF)
    before = dot(earlier, (hits[0] + hits[1]).astype(BF))
    near_lane = lax.broadcasted_iota(jnp.int32, (every, NEAR * TWO), 1)
    far_lane = lax.broadcasted_iota(jnp.int32, (2 * TOK, NEAR * ONE), 1)
    near_place = jnp.zeros((every, NEAR * TWO), F32)
    near_weight = jnp.zeros((every, NEAR * TWO), F32)
    far_place = jnp.zeros((2 * TOK, NEAR * ONE), F32)
    far_weight = jnp.zeros((2 * TOK, NEAR * ONE), F32)
    for r in range(2):
        slot = jnp.sum(before * hits[r], axis=1, keepdims=True).astype(jnp.int32) + side * CAP
        weight = info[:, 2 + r : 3 + r]
        near_at = jnp.where(rel[r] < NEAR, rel[r] * TWO + away * ONE + slot, -1)
        far_at = jnp.where(rel[r] >= NEAR, (rel[r] - NEAR) * ONE + slot, -1)[: 2 * TOK]
        near_here = near_at == near_lane
        far_here = far_at == far_lane
        near_place = near_place + jnp.where(near_here, 1.0, 0.0)
        near_weight = near_weight + jnp.where(near_here, weight, 0.0)
        far_place = far_place + jnp.where(far_here, 1.0, 0.0)
        far_weight = far_weight + jnp.where(far_here, weight[: 2 * TOK], 0.0)
    for value, high, low in ((near_weight, wnh, wnl), (far_weight, wch, wcl)):
        top = value.astype(BF)
        high[...] = top
        low[...] = (value - top.astype(F32)).astype(BF)
    pn[...] = near_place.T.astype(BF)
    placing = far_place.T.astype(BF)

    toks[0].wait_recv()
    for col in range(0, H, COLS):
        rows = jnp.concatenate([nb[g, :, col : col + COLS] for g in range(2)], axis=0)
        sc[:, col : col + COLS] = dot(placing, rows).astype(BF)
    far_in = [
        send(sc.at[pl.ds(d * ONE, ONE)], xf.at[c, pl.ds((NEAR + d) * TWO, ONE)], (flip(e, NEAR + d), t))
        for d in range(NEAR)
    ]

    heads, dk, dv = z.heads, z.dk, z.dv
    size = heads * dk
    run = decay_ref[...]
    along = lax.broadcasted_iota(jnp.int32, run.shape, 1) % BLOCK
    step = 1
    while step < BLOCK:
        run = run + jnp.where(along >= step, pltpu.roll(run, step, 1), 0.0)
        step *= 2
    for b in range(z.blocks):
        part = run[:, b * BLOCK : (b + 1) * BLOCK]
        run_v[b] = part
        runt_v[b] = jnp.concatenate([part] * (8 // heads), axis=0).T

    def tables(b):
        at = e * z.blocks + b
        cos_b = base_ref[0, pl.ds(at, 1), :]
        sin_b = base_ref[1, pl.ds(at, 1), :]
        cos = cos_b * spin_ref[0] - sin_b * spin_ref[1]
        sin = sin_b * spin_ref[0] + cos_b * spin_ref[1]
        lane = lax.broadcasted_iota(jnp.int32, sin.shape, 1)
        return cos, jnp.where(lane % dk < dk // 2, -sin, sin)

    loads["k"].wait()
    loads["v"].wait()
    state = [jnp.zeros((dk, dv), F32)] * heads
    total = [jnp.zeros((1, 1), F32)] * heads
    for b in range(z.blocks):
        at = slice(b * BLOCK, (b + 1) * BLOCK)
        cos, sin = tables(b)
        kt = (turn(k_v[at, :].astype(F32), cos, sin, dk) * dk ** (-0.5)).T
        keyt[b] = kt.astype(BF)
        for h in range(heads):
            rows = slice(h * dk, (h + 1) * dk)
            run_row = run_v[b, h : h + 1, :]
            closing = run_row[:, BLOCK - 1 : BLOCK]
            scaled = (kt[rows, :] * jnp.exp(closing - run_row)).astype(BF)
            new = dot(scaled, v_v[at, h * dv : (h + 1) * dv])
            upd[b, rows, :] = new
            state[h] = state[h] * jnp.exp(closing) + new
            total[h] = total[h] + closing
    group = jnp.concatenate(state, axis=0)
    fade = jnp.concatenate([jnp.broadcast_to(jnp.exp(x), (dk, dv)) for x in total], axis=0)
    prefix = jnp.zeros((size, dv), F32)
    prefade = jnp.ones((size, dv), F32)
    scans = []

    def scan_send(s):
        pack_s[s, 0:size] = group.astype(BF)
        pack_s[s, size:] = fade.astype(BF)
        scans.append(send(pack_s.at[s], pack_r.at[s], (flip(e, 1 << s), t)))

    def scan_recv(s, group, fade, prefix, prefade):
        scans[s].wait_recv()
        other = pack_r[s, 0:size].astype(F32)
        other_fade = pack_r[s, size:].astype(F32)
        later = lax.rem(lax.div(e, 1 << s), 2) == 1
        prefix = jnp.where(later, prefix + prefade * other, prefix)
        prefade = jnp.where(later, prefade * other_fade, prefade)
        group = jnp.where(later, other * fade + group, group * other_fade + other)
        return group, fade * other_fade, prefix, prefade

    scan_send(0)

    toks[1].wait_recv()
    toks[2].wait_recv()
    for col in range(0, H, COLS):
        rows = jnp.concatenate([nb[g, :, col : col + COLS] for g in range(4)], axis=0)
        made = dot(pn[...], rows).astype(BF)
        xf[c, 0:TWO, col : col + COLS] = made[0:TWO]
        sn[:, col : col + COLS] = made[TWO:]
    near_in = [None] + [
        send(sn.at[pl.ds((d - 1) * TWO, TWO)], xf.at[c, pl.ds(d * TWO, TWO)], (flip(e, d), t))
        for d in range(1, NEAR)
    ]

    for s in range(1, z.stages):
        group, fade, prefix, prefade = scan_recv(s - 1, group, fade, prefix, prefade)
        scan_send(s)

    pairs = {}

    def to_pair(at, count):
        where = xf.at[c, pl.ds(at, count)]
        pairs[at] = send(where, where, pair)

    to_pair(0, TWO)
    far_x = {}

    def relay(d):
        far_in[d].wait_recv()
        at = (NEAR + d) * TWO
        far_x[d] = send(xf.at[c, pl.ds(at, ONE)], xf.at[c, pl.ds(at + ONE, ONE)], cross)
        to_pair(at, ONE)

    def relay_on(d):
        far_x[d].wait_recv()
        to_pair((NEAR + d) * TWO + ONE, ONE)

    def relay_near(d):
        near_in[d].wait_recv()
        to_pair(d * TWO, TWO)

    own_gate, near_gate, far_gate = [], [], []

    def mix(b, state):
        at = slice(b * BLOCK, (b + 1) * BLOCK)
        cos, sin = tables(b)
        q = turn(q_v[at, :].astype(F32), cos, sin, dk)
        row = lax.broadcasted_iota(jnp.int32, (BLOCK, BLOCK), 0)
        col = lax.broadcasted_iota(jnp.int32, (BLOCK, BLOCK), 1)
        causal = row >= col
        after = []
        for h in range(heads):
            rows = slice(h * dk, (h + 1) * dk)
            run_row = run_v[b, h : h + 1, :]
            run_col = runt_v[b, :, h : h + 1]
            closing = run_row[:, BLOCK - 1 : BLOCK]
            qh = q[:, rows]
            vh = v_v[at, h * dv : (h + 1) * dv]
            weights = jnp.where(causal, jnp.exp(jnp.where(causal, run_col - run_row, 0.0)), 0.0)
            scores = dot(qh.astype(BF), keyt[b, rows, :]) * weights
            out = dot(scores.astype(BF), vh)
            carried = state[rows, :]
            out = out + dot((qh * jnp.exp(run_col)).astype(BF), carried.astype(BF))
            after.append(carried * jnp.exp(closing) + upd[b, rows, :])
            centered = out - jnp.mean(out, axis=-1, keepdims=True)
            variance = jnp.mean(centered * centered, axis=-1, keepdims=True)
            gate = g_v[at, h * dv : (h + 1) * dv].astype(F32)
            act = gate / (1.0 + jnp.exp(-gate))
            gate_all[0, at, h * dv : (h + 1) * dv] = (act * (centered * lax.rsqrt(variance + 1e-06))).astype(BF)
        return jnp.concatenate(after, axis=0)

    def gate_x(b):
        at = pl.ds(b * BLOCK, BLOCK)
        far_gate.append(send(gate_all.at[0, at], gate_all.at[2, at], cross))
        near_gate.append(send(gate_all.at[0, at], gate_all.at[1, at], pair))

    last_gate = []

    def gate_on(b):
        far_gate[b].wait_recv()
        at = pl.ds(b * BLOCK, BLOCK)
        last_gate.append(send(gate_all.at[2, at], gate_all.at[3, at], pair))

    stores = []

    def project(b):
        near_gate[b].wait_recv()
        last_gate[b].wait_recv()
        at = slice(b * BLOCK, (b + 1) * BLOCK)
        sum_ = dot(gate_all[0, at], wo_v[t])
        for g in range(1, 4):
            sum_ = sum_ + dot(gate_all[g, at], wo_v[flip(t, g)])
        mix_v[at, :] = sum_.astype(BF)
        at = pl.ds(b * BLOCK, BLOCK)
        copy = pltpu.make_async_copy(mix_v.at[at], mixed_hbm.at[at], out_sem.at[len(stores)])
        copy.start()
        stores.append(copy)

    quarter = z.ep // 4
    trade = {}

    def ffn(part):
        at = part * quarter * TWO
        count = quarter * TWO
        rows = slice(at, at + count)
        gate = dot(xf[0, rows], wg_v[0:H]) + dot(xf[1, rows], wg_v[H:])
        up = dot(xf[0, rows], wu_v[0:H]) + dot(xf[1, rows], wu_v[H:])
        hidden = (gate * up / (1.0 + jnp.exp(-gate))).astype(BF)
        ys[rows] = dot(hidden, wd_v[o]).astype(BF)
        where = pl.ds(at, count)
        trade[part] = send(ys.at[where], yr.at[where], pair)
        yk[rows] = dot(hidden, wd_v[c]).astype(BF)

    def wait_pairs(part):
        for d in range(part * quarter, (part + 1) * quarter):
            pairs[d * TWO].wait_recv()
            if d >= NEAR:
                pairs[d * TWO + ONE].wait_recv()

    def core_sum(part):
        trade[part].wait_recv()
        at = part * quarter * TWO
        rows = slice(at, at + quarter * TWO)
        yk[rows] = (yk[rows].astype(F32) + yr[rows].astype(F32)).astype(BF)

    near_out, far_sum, far_out = {}, {}, {}

    def near_back(part):
        core_sum(part)
        for d in range(part * quarter, (part + 1) * quarter):
            if d:
                at = pl.ds(d * TWO, TWO)
                near_out[d] = send(yk.at[at], rn.at[pl.ds((d - 1) * TWO, TWO)], (flip(e, d), t))

    def far_back(part):
        core_sum(part)
        for d in range(part * quarter - NEAR, (part + 1) * quarter - NEAR):
            at = (NEAR + d) * TWO + ONE
            far_sum[d] = send(yk.at[pl.ds(at, ONE)], xr.at[pl.ds(d * ONE, ONE)], cross)

    def far_home(part):
        for d in range(part * quarter - NEAR, (part + 1) * quarter - NEAR):
            far_sum[d].wait_recv()
            at = (NEAR + d) * TWO
            rows = slice(d * ONE, (d + 1) * ONE)
            zc[rows] = (yk[at : at + ONE].astype(F32) + xr[rows].astype(F32)).astype(BF)
            far_out[d] = send(zc.at[pl.ds(d * ONE, ONE)], rc.at[pl.ds(d * ONE, ONE)], (flip(e, NEAR + d), t))

    first = list(range(quarter))
    second = list(range(quarter, NEAR))
    front, back = first[: len(first) // 2], first[len(first) // 2 :]
    for d in front:
        relay(d)
    group, fade, prefix, prefade = scan_recv(z.stages - 1, group, fade, prefix, prefade)
    loads["q"].wait()
    loads["g"].wait()
    state = mix(0, prefix)
    for d in back:
        relay(d)
    gate_x(0)
    state = mix(1, state)
    for d in first:
        relay_on(d)
    for name in ("wg", "wu", "wd0", "wd1"):
        loads[name].wait()
    wait_pairs(2)
    ffn(2)
    for d in range(1, quarter):
        relay_near(d)
    far_back(2)
    gate_x(1)
    front, back = second[: len(second) // 2], second[len(second) // 2 :]
    for d in front:
        relay(d)
    wait_pairs(0)
    ffn(0)
    for d in range(quarter, NEAR):
        relay_near(d)
    far_home(2)
    near_back(0)
    wait_pairs(1)
    ffn(1)
    state = mix(2, state)
    near_back(1)
    for d in back:
        relay(d)
    gate_x(2)
    mix(3, state)
    for d in second:
        relay_on(d)
    wait_pairs(3)
    ffn(3)
    far_back(3)
    gate_x(3)
    loads["wo"].wait()
    gate_on(0)
    gate_on(1)
    project(0)
    far_home(3)
    gate_on(2)
    project(1)
    project(2)

    for d in range(1, NEAR):
        near_out[d].wait_recv()
    for col in range(0, H, COLS):
        at = slice(col, col + COLS)
        total = dot(wnh[:, 0:TWO], yk[0:TWO, at]) + dot(wnl[:, 0:TWO], yk[0:TWO, at])
        total = total + dot(wnh[:, TWO:], rn[:, at]) + dot(wnl[:, TWO:], rn[:, at])
        own[:, at] = total[: 2 * TOK]
        fxs[:, at] = total[2 * TOK :].astype(BF)
    last = send(fxs, fxr, cross)
    gate_on(3)
    project(3)
    for d in range(NEAR):
        far_out[d].wait_recv()
    last.wait_recv()
    for col in range(0, H, COLS):
        at = slice(col, col + COLS)
        total = dot(wch[...], rc[:, at]) + dot(wcl[...], rc[:, at])
        total = total + own[:, at] + fxr[:, at].astype(F32)
        fin[0, :, at] = total[:TOK].astype(BF)
        fin[1, :, at] = total[TOK:].astype(BF)
    mine = pl.ds(pl.multiple_of(c * H, H), H)
    done = send(fin.at[o], moe_hbm.at[:, mine], pair)
    copy = pltpu.make_async_copy(fin.at[c], moe_hbm.at[:, mine], out_sem.at[len(stores)])
    copy.start()
    stores.append(copy)
    done.wait_recv()
    for copy in stores:
        copy.wait()
    for copy in sent:
        copy.wait_send()


def copies(z):
    return 6 + z.near * 2 + z.stages + z.near * 3 + 3 * z.blocks + 4 + 3 * z.near + 8


def per_device(
    query, keys, values, gate_pre, log_decay, out_weight, expert_input, norm_gain, routes,
    route_weights, w_gate, w_up, w_down,
):
    rows, heads = query.shape[0], log_decay.shape[0]
    dk, dv = query.shape[1] // heads, values.shape[1] // heads
    tokens, width = expert_input.shape
    hidden, features = w_gate.shape[2], out_weight.shape[1]
    ep, tp = lax.axis_size("ep"), lax.axis_size("tp")
    z = Sizes(ep, tokens, width, routes.shape[1], rows, heads, dk, dv, hidden, features)
    inverse = (1.0 / 10000.0 ** np.linspace(0.0, 1.0, dk // 2)).astype(np.float32).astype(np.float64)
    inverse = np.tile(inverse, 128 // (dk // 2))
    spin = np.arange(BLOCK)[:, None] * inverse[None, :]
    base = (np.arange(ep * z.blocks) * BLOCK)[:, None] * inverse[None, :]
    spin = jnp.asarray(np.stack([np.cos(spin), np.sin(spin)]).astype(np.float32))
    base = jnp.asarray(np.stack([np.cos(base), np.sin(base)]).astype(np.float32))
    H, ONE, TWO, NEAR = z.half, z.one, z.two, z.near
    size = heads * dk
    depth = heads * dv
    inside = pl.BlockSpec(memory_space=VM)
    outside = pl.BlockSpec(memory_space=ANY)
    scratch = [
        VM((rows, size), BF), VM((rows, size), BF), VM((rows, depth), BF), VM((rows, depth), BF),
        VM((tp, depth, features), BF), VM((tokens, width), BF),
        VM((width, hidden), BF), VM((width, hidden), BF), VM((2, hidden, H), BF),
        VM((2, tokens, H), BF), VM((4, tokens, H), BF), VM((4, tokens, 128), F32),
        VM(((NEAR - 1) * TWO, H), BF), VM((NEAR * ONE, H), BF), VM((2, ep * TWO, H), BF),
        VM((ep * TWO, H), BF), VM((ep * TWO, H), BF), VM((ep * TWO, H), BF),
        VM((NEAR * ONE, H), BF), VM((NEAR * ONE, H), BF),
        VM(((NEAR - 1) * TWO, H), BF), VM((NEAR * ONE, H), BF),
        VM((2 * tokens, H), F32), VM((2 * tokens, H), BF), VM((2 * tokens, H), BF), VM((2, tokens, H), BF),
        VM((4 * tokens, NEAR * TWO), BF), VM((4 * tokens, NEAR * TWO), BF),
        VM((2 * tokens, NEAR * ONE), BF), VM((2 * tokens, NEAR * ONE), BF),
        VM((NEAR * TWO, 4 * tokens), BF),
        VM((z.blocks, size, BLOCK), BF), VM((z.blocks, size, dv), F32),
        VM((z.blocks, heads, BLOCK), F32), VM((z.blocks, BLOCK, 8), F32),
        VM((z.stages, 2 * size, dv), BF), VM((z.stages, 2 * size, dv), BF), VM((size, dv), F32),
        VM((4, rows, depth), BF), VM((rows, features), BF),
        DMA((10,)), DMA((copies(z),)), DMA((copies(z),)), DMA((z.blocks + 1,)),
    ]
    return pl.pallas_call(
        functools.partial(kernel, z),
        in_specs=[outside] * 4 + [inside, outside, outside] + [inside] * 3 + [outside] * 3 + [inside] * 2,
        out_specs=[outside, outside],
        out_shape=[
            jax.ShapeDtypeStruct((rows, features), BF),
            jax.ShapeDtypeStruct((tokens, width), BF),
        ],
        scratch_shapes=scratch,
        compiler_params=pltpu.CompilerParams(
            collective_id=0, has_side_effects=True, vmem_limit_bytes=67043328
        ),
        cost_estimate=pl.CostEstimate(flops=10**10, bytes_accessed=20 << 20, transcendentals=0),
    )(
        query, keys, values, gate_pre, log_decay, out_weight.reshape(tp, depth, features), expert_input,
        norm_gain.reshape(1, width), routes, route_weights, w_gate, w_up, w_down, spin, base,
    )


def solution(mesh):
    placed = (
        P("ep", "tp"),
        P("ep", "tp"),
        P("ep", "tp"),
        P("ep", "tp"),
        P("tp", "ep"),
        P(None, "tp"),
        P(("ep", "tp"), None),
        P(),
        P(("ep", "tp"), None),
        P(("ep", "tp"), None),
        P("ep", None, "tp"),
        P("ep", None, "tp"),
        P("ep", "tp", None),
    )
    return jax.shard_map(
        per_device,
        mesh=mesh,
        in_specs=placed,
        out_specs=(P("ep", "tp"), P(("ep", "tp"), None)),
        check_vma=False,
    )
```

```python
import functools
import jax
import jax.numpy as jnp
import numpy as np
from jax import lax
from jax.experimental import pallas as pl
from jax.experimental.pallas import tpu as pltpu
from jax.sharding import PartitionSpec as P

BF = jnp.bfloat16
F32 = jnp.float32
VM = pltpu.VMEM
ANY = pl.ANY
MESH = pl.DeviceIdType.MESH
DMA = pltpu.SemaphoreType.DMA
BLOCK = 256
COLS = 512


def flip(index, bits):
    out = index
    bit = 1
    while bit <= bits:
        if bits & bit:
            out = out + bit - 2 * bit * lax.rem(lax.div(index, bit), 2)
        bit *= 2
    return out


phase = jax.named_scope


def dot(a, b):
    return jnp.dot(a, b, preferred_element_type=F32)


def turn(x, cos, sin, head_dim):
    width = x.shape[1]
    half = head_dim // 2
    lane = lax.broadcasted_iota(jnp.int32, x.shape, 1)
    first = lane % head_dim < half
    other = jnp.where(first, pltpu.roll(x, width - half, 1), pltpu.roll(x, half, 1))
    reps = width // cos.shape[1]
    return x * jnp.concatenate([cos] * reps, axis=1) + other * jnp.concatenate([sin] * reps, axis=1)


class Sizes:
    def __init__(self, ep, tokens, width, top, rows, heads, dk, dv, hidden, features):
        self.ep, self.tokens, self.width, self.top = ep, tokens, width, top
        self.rows, self.heads, self.dk, self.dv = rows, heads, dk, dv
        self.hidden, self.features = hidden, features
        self.half = width // 2
        self.cap = 3 * tokens * top // (2 * ep)
        self.one = -(-2 * self.cap // 16) * 16
        self.two = 2 * self.one
        self.near = ep // 2
        self.blocks = rows // BLOCK
        self.stages = ep.bit_length() - 1


def kernel(
    z,
    q_hbm, k_hbm, v_hbm, g_hbm, decay_ref, wo_hbm, tok_hbm, gain_ref, routes_ref, rweight_ref,
    wg_hbm, wu_hbm, wd_hbm, spin_ref, base_ref,
    mixed_hbm, moe_hbm,
    q_v, k_v, v_v, g_v, wo_v, tok_v, wg_v, wu_v, wd_v,
    nh, nb, meta, sn, sc, xf, yk, ys, yr, xr, zc, rc, fin,
    wch, wcl, pn, keyt, upd, run_v, runt_v, pack_s, pack_r, pre_v, gate_all, mix_v,
    load_sem, send_sem, recv_sem, out_sem,
):
    e = lax.axis_index("ep")
    t = lax.axis_index("tp")
    c = lax.rem(t, 2)
    o = 1 - c
    pair = (e, flip(t, 1))
    cross = (e, flip(t, 2))
    diag = (e, flip(t, 3))
    H, ONE, TWO, NEAR, TOK, CAP = z.half, z.one, z.two, z.near, z.tokens, z.cap
    used = [0]
    sent = []

    barrier = pltpu.get_barrier_semaphore()
    peers = [(flip(e, d), t) for d in range(1, z.ep)] + [pair, cross, diag]
    for peer in peers:
        pl.semaphore_signal(barrier, inc=1, device_id=peer, device_id_type=MESH)

    loads = {}

    def load(name, src, dst):
        copy = pltpu.make_async_copy(src, dst, load_sem.at[len(loads)])
        copy.start()
        loads[name] = copy

    load("tok", tok_hbm, tok_v)
    load("k", k_hbm, k_v)
    load("v", v_hbm, v_v)
    load("q", q_hbm, q_v)
    load("g", g_hbm, g_v)
    load("wg", wg_hbm.at[0], wg_v)
    load("wu", wu_hbm.at[0], wu_v)
    for h in range(2):
        load("wd%d" % h, wd_hbm.at[0, :, pl.ds(h * H, H)], wd_v.at[h])
    load("wo", wo_hbm, wo_v)

    def send(src, dst, device):
        i = used[0]
        used[0] += 1
        copy = pltpu.make_async_remote_copy(
            src_ref=src, dst_ref=dst, send_sem=send_sem.at[i], recv_sem=recv_sem.at[i],
            device_id=device, device_id_type=MESH,
        )
        copy.start()
        sent.append(copy)
        return copy

    both = jnp.concatenate([routes_ref[...].astype(F32), rweight_ref[...]], axis=0)
    meta[c] = jnp.concatenate([both] * (8 // both.shape[0]), axis=0)

    with phase("wait_tok"):
        loads["tok"].wait()
    x = tok_v[...].astype(F32)
    centered = x - jnp.mean(x, axis=-1, keepdims=True)
    variance = jnp.mean(centered * centered, axis=-1, keepdims=True)
    normed = (centered * lax.rsqrt(variance + 1e-05) * gain_ref[...]).astype(BF)
    nh[0] = normed[:, :H]
    nh[1] = normed[:, H:]
    heads, dk, dv = z.heads, z.dk, z.dv
    size = heads * dk
    run = decay_ref[...]
    along = lax.broadcasted_iota(jnp.int32, run.shape, 1) % BLOCK
    step = 1
    while step < BLOCK:
        run = run + jnp.where(along >= step, pltpu.roll(run, step, 1), 0.0)
        step *= 2
    for b in range(z.blocks):
        part = run[:, b * BLOCK : (b + 1) * BLOCK]
        run_v[b] = part
        runt_v[b] = jnp.concatenate([part] * (8 // heads), axis=0).T

    def tables(b):
        at = e * z.blocks + b
        cos_b = base_ref[0, pl.ds(at, 1), :]
        sin_b = base_ref[1, pl.ds(at, 1), :]
        cos = cos_b * spin_ref[0] - sin_b * spin_ref[1]
        sin = sin_b * spin_ref[0] + cos_b * spin_ref[1]
        lane = lax.broadcasted_iota(jnp.int32, sin.shape, 1)
        return cos, jnp.where(lane % dk < dk // 2, -sin, sin)

    loads["k"].wait()
    loads["v"].wait()
    state = [jnp.zeros((dk, dv), F32)] * heads
    total = [jnp.zeros((1, 1), F32)] * heads
    for b in range(z.blocks):
        at = slice(b * BLOCK, (b + 1) * BLOCK)
        cos, sin = tables(b)
        kt = (turn(k_v[at, :].astype(F32), cos, sin, dk) * dk ** (-0.5)).T
        keyt[b] = kt.astype(BF)
        for h in range(heads):
            rows = slice(h * dk, (h + 1) * dk)
            run_row = run_v[b, h : h + 1, :]
            closing = run_row[:, BLOCK - 1 : BLOCK]
            scaled = (kt[rows, :] * jnp.exp(closing - run_row)).astype(BF)
            new = dot(scaled, v_v[at, h * dv : (h + 1) * dv])
            upd[b, rows, :] = new
            state[h] = state[h] * jnp.exp(closing) + new
            total[h] = total[h] + closing
    group = jnp.concatenate(state, axis=0)
    fade = [jnp.broadcast_to(jnp.exp(x), (1, dv)) for x in total]
    prefix = jnp.zeros((size, dv), F32)
    prefade = jnp.ones((size, dv), F32)
    scans = []

    def spread(fade):
        return jnp.concatenate([jnp.broadcast_to(x, (dk, dv)) for x in fade], axis=0)

    @phase("scan_send")
    def scan_send(s):
        pack_s[s, 0:size] = group.astype(BF)
        pack_s[s, size:] = jnp.concatenate(fade * (16 // heads), axis=0).astype(BF)
        scans.append(send(pack_s.at[s], pack_r.at[s], (flip(e, 1 << s), t)))

    @phase("scan_recv")
    def scan_recv(s, group, fade, prefix, prefade):
        scans[s].wait_recv()
        other = pack_r[s, 0:size].astype(F32)
        rows = pack_r[s, size:].astype(F32)
        other_fade = [rows[h : h + 1] for h in range(heads)]
        all_fade = spread(other_fade)
        later = lax.rem(lax.div(e, 1 << s), 2) == 1
        prefix = jnp.where(later, prefix + prefade * other, prefix)
        prefade = jnp.where(later, prefade * all_fade, prefade)
        group = jnp.where(later, other * spread(fade) + group, group * all_fade + other)
        return group, [a * b for a, b in zip(fade, other_fade)], prefix, prefade

    with phase("barrier"):
        pl.semaphore_wait(barrier, len(peers))
    metas = [
        send(meta.at[c], meta.at[c], pair),
        send(meta.at[c], meta.at[2 + c], cross),
        send(meta.at[c], meta.at[2 + c], diag),
    ]
    toks = [
        send(nh.at[o], nb.at[c], pair),
        send(nh.at[c], nb.at[2 + c], cross),
        send(nh.at[o], nb.at[2 + c], diag),
    ]
    scan_send(0)
    nb[c] = nh[c]


    with phase("wait_metas"):
        for copy in metas:
            copy.wait_recv()
    every = 4 * TOK
    info = jnp.concatenate([meta[g].T for g in range(4)], axis=0)
    number = lax.broadcasted_iota(jnp.int32, (every, 128), 1)
    token = lax.broadcasted_iota(jnp.int32, (every, 1), 0)
    away = lax.div(token, 2 * TOK)
    side = lax.rem(lax.div(token, TOK), 2)
    rel = [jnp.bitwise_xor(info[:, r : r + 1].astype(jnp.int32), e) for r in range(2)]
    hits = [(rel[r] == number).astype(F32) for r in range(2)]
    i = lax.broadcasted_iota(jnp.int32, (every, every), 0)
    j = lax.broadcasted_iota(jnp.int32, (every, every), 1)
    earlier = ((j < i) & (lax.div(i, TOK) == lax.div(j, TOK))).astype(F32).astype(BF)
    before = dot(earlier, (hits[0] + hits[1]).astype(BF))
    near_lane = lax.broadcasted_iota(jnp.int32, (every, NEAR * TWO), 1)
    far_lane = lax.broadcasted_iota(jnp.int32, (2 * TOK, NEAR * ONE), 1)
    near_place = jnp.zeros((every, NEAR * TWO), F32)
    far_place = jnp.zeros((2 * TOK, NEAR * ONE), F32)
    all_lane = lax.broadcasted_iota(jnp.int32, (2 * TOK, z.ep * ONE), 1)
    all_weight = jnp.zeros((2 * TOK, z.ep * ONE), F32)
    for r in range(2):
        slot = jnp.sum(before * hits[r], axis=1, keepdims=True).astype(jnp.int32) + side * CAP
        weight = info[: 2 * TOK, 2 + r : 3 + r]
        near_at = jnp.where(rel[r] < NEAR, rel[r] * TWO + away * ONE + slot, -1)
        far_at = jnp.where(rel[r] >= NEAR, (rel[r] - NEAR) * ONE + slot, -1)[: 2 * TOK]
        near_here = near_at == near_lane
        far_here = far_at == far_lane
        near_place = near_place + jnp.where(near_here, 1.0, 0.0)
        all_at = (rel[r] * ONE + slot)[: 2 * TOK]
        all_weight = all_weight + jnp.where(all_at == all_lane, weight, 0.0)
        far_place = far_place + jnp.where(far_here, 1.0, 0.0)
    top = all_weight.astype(BF)
    wch[...] = top
    wcl[...] = (all_weight - top.astype(F32)).astype(BF)
    pn[...] = near_place.T.astype(BF)
    placing = far_place.T.astype(BF)

    with phase("wait_pair_tok"):
        toks[0].wait_recv()
    for col in range(0, H, COLS):
        rows = jnp.concatenate([nb[g, :, col : col + COLS] for g in range(2)], axis=0)
        sc[:, col : col + COLS] = dot(placing, rows).astype(BF)
    far_in = {}

    def far_send(d):
        far_in[d] = send(
            sc.at[pl.ds(d * ONE, ONE)], xf.at[c, pl.ds((NEAR + d) * TWO, ONE)], (flip(e, NEAR + d), t)
        )

    quarter = z.ep // 4
    first = list(range(quarter))
    second = list(range(quarter, NEAR))
    cut = max(1, quarter // 2)
    for s in range(1, z.stages):
        group, fade, prefix, prefade = scan_recv(s - 1, group, fade, prefix, prefade)
        scan_send(s)

    pairs = {}

    def to_pair(at, count):
        where = xf.at[c, pl.ds(at, count)]
        pairs[at] = send(where, where, pair)

    far_x = {}

    @phase("relay")
    def relay(d):
        far_in[d].wait_recv()
        at = (NEAR + d) * TWO
        far_x[d] = send(xf.at[c, pl.ds(at, ONE)], xf.at[c, pl.ds(at + ONE, ONE)], cross)
        to_pair(at, ONE)

    @phase("relay_on")
    def relay_on(d):
        far_x[d].wait_recv()
        to_pair((NEAR + d) * TWO + ONE, ONE)

    @phase("relay_near")
    def relay_near(d):
        near_in[d].wait_recv()
        to_pair(d * TWO, TWO)

    own_gate, near_gate, far_gate = [], [], []

    @phase("mix")
    def mix(b, state):
        at = slice(b * BLOCK, (b + 1) * BLOCK)
        cos, sin = tables(b)
        q = turn(q_v[at, :].astype(F32), cos, sin, dk)
        row = lax.broadcasted_iota(jnp.int32, (BLOCK, BLOCK), 0)
        col = lax.broadcasted_iota(jnp.int32, (BLOCK, BLOCK), 1)
        causal = row >= col
        after = []
        for h in range(heads):
            rows = slice(h * dk, (h + 1) * dk)
            run_row = run_v[b, h : h + 1, :]
            run_col = runt_v[b, :, h : h + 1]
            closing = run_row[:, BLOCK - 1 : BLOCK]
            qh = q[:, rows]
            vh = v_v[at, h * dv : (h + 1) * dv]
            weights = jnp.where(causal, jnp.exp(jnp.where(causal, run_col - run_row, 0.0)), 0.0)
            scores = dot(qh.astype(BF), keyt[b, rows, :]) * weights
            out = dot(scores.astype(BF), vh)
            carried = state[rows, :]
            out = out + dot((qh * jnp.exp(run_col)).astype(BF), carried.astype(BF))
            after.append(carried * jnp.exp(closing) + upd[b, rows, :])
            centered = out - jnp.mean(out, axis=-1, keepdims=True)
            variance = jnp.mean(centered * centered, axis=-1, keepdims=True)
            gate = g_v[at, h * dv : (h + 1) * dv].astype(F32)
            act = gate / (1.0 + jnp.exp(-gate))
            gate_all[0, at, h * dv : (h + 1) * dv] = (act * (centered * lax.rsqrt(variance + 1e-06))).astype(BF)
        return jnp.concatenate(after, axis=0)

    @phase("gate_x")
    def gate_x(b):
        at = pl.ds(b * BLOCK, BLOCK)
        far_gate.append(send(gate_all.at[0, at], gate_all.at[2, at], cross))
        near_gate.append(send(gate_all.at[0, at], gate_all.at[1, at], pair))

    last_gate = []

    @phase("gate_on")
    def gate_on(b):
        far_gate[b].wait_recv()
        at = pl.ds(b * BLOCK, BLOCK)
        last_gate.append(send(gate_all.at[2, at], gate_all.at[3, at], pair))

    stores = []

    @phase("project")
    def project(b):
        near_gate[b].wait_recv()
        last_gate[b].wait_recv()
        at = slice(b * BLOCK, (b + 1) * BLOCK)
        sum_ = dot(gate_all[0, at], wo_v[t])
        for g in range(1, 4):
            sum_ = sum_ + dot(gate_all[g, at], wo_v[flip(t, g)])
        mix_v[at, :] = sum_.astype(BF)
        at = pl.ds(b * BLOCK, BLOCK)
        copy = pltpu.make_async_copy(mix_v.at[at], mixed_hbm.at[at], out_sem.at[len(stores)])
        copy.start()
        stores.append(copy)

    trade = {}

    @phase("ffn")
    def ffn(part):
        at = part * quarter * TWO
        count = quarter * TWO
        rows = slice(at, at + count)
        gate = dot(xf[0, rows], wg_v[0:H]) + dot(xf[1, rows], wg_v[H:])
        up = dot(xf[0, rows], wu_v[0:H]) + dot(xf[1, rows], wu_v[H:])
        hidden = (gate * up / (1.0 + jnp.exp(-gate))).astype(BF)
        ys[rows] = dot(hidden, wd_v[o]).astype(BF)
        where = pl.ds(at, count)
        trade[part] = send(ys.at[where], yr.at[where], pair)
        yk[rows] = dot(hidden, wd_v[c]).astype(BF)

    @phase("wait_pairs")
    def wait_pairs(part):
        for d in range(part * quarter, (part + 1) * quarter):
            pairs[d * TWO].wait_recv()
            if d >= NEAR:
                pairs[d * TWO + ONE].wait_recv()

    @phase("core_sum")
    def core_sum(part):
        trade[part].wait_recv()
        at = part * quarter * TWO
        rows = slice(at, at + quarter * TWO)
        yk[rows] = (yk[rows].astype(F32) + yr[rows].astype(F32)).astype(BF)

    cross_sum, home_out = {}, {}

    @phase("back")
    def back(part):
        core_sum(part)
        for d in range(part * quarter, (part + 1) * quarter):
            cross_sum[d] = send(yk.at[pl.ds(d * TWO + ONE, ONE)], xr.at[pl.ds(d * ONE, ONE)], cross)

    @phase("home")
    def home(part):
        for d in range(part * quarter, (part + 1) * quarter):
            cross_sum[d].wait_recv()
            rows = slice(d * ONE, (d + 1) * ONE)
            full = (yk[d * TWO : d * TWO + ONE].astype(F32) + xr[rows].astype(F32)).astype(BF)
            if d == 0:
                rc[rows] = full
            else:
                zc[rows] = full
                home_out[d] = send(zc.at[pl.ds(d * ONE, ONE)], rc.at[pl.ds(d * ONE, ONE)], (flip(e, d), t))

    group, fade, prefix, prefade = scan_recv(z.stages - 1, group, fade, prefix, prefade)
    for d in first:
        far_send(d)
    with phase("wait_qg"):
        loads["q"].wait()
        loads["g"].wait()
    state = mix(0, prefix)
    gate_x(0)

    with phase("wait_x_tok"):
        toks[1].wait_recv()
        toks[2].wait_recv()
    for col in range(0, H, COLS):
        rows = jnp.concatenate([nb[g, :, col : col + COLS] for g in range(4)], axis=0)
        made = dot(pn[...], rows).astype(BF)
        xf[c, 0:TWO, col : col + COLS] = made[0:TWO]
        sn[:, col : col + COLS] = made[TWO:]
    near_in = {}
    for d in range(1, NEAR):
        near_in[d] = send(sn.at[pl.ds((d - 1) * TWO, TWO)], xf.at[c, pl.ds(d * TWO, TWO)], (flip(e, d), t))
        if d == NEAR - 2:
            for i in second[:cut]:
                far_send(i)
    for i in second[cut:]:
        far_send(i)
    to_pair(0, TWO)

    state = mix(1, state)
    gate_x(1)
    state = mix(2, state)
    for d in first[:cut]:
        relay(d)
    mix(3, state)
    with phase("wait_w"):
        for name in ("wg", "wu", "wd0", "wd1"):
            loads[name].wait()
    for d in first[cut:]:
        relay(d)
    gate_x(2)
    for d in first:
        relay_on(d)
    wait_pairs(2)
    ffn(2)
    for d in range(1, quarter):
        relay_near(d)
    back(2)
    wait_pairs(0)
    ffn(0)
    for d in second:
        relay(d)
    for d in range(quarter, NEAR):
        relay_near(d)
    home(2)
    back(0)
    for d in second:
        relay_on(d)
    wait_pairs(3)
    ffn(3)
    wait_pairs(1)
    ffn(1)
    back(3)
    back(1)
    gate_x(3)
    home(0)
    with phase("wait_wo"):
        loads["wo"].wait()
    for b in range(3):
        gate_on(b)
    project(0)
    home(3)
    project(1)
    home(1)
    project(2)

    with phase("wait_home"):
        for d in range(1, z.ep):
            home_out[d].wait_recv()
    for col in range(0, H, COLS):
        at = slice(col, col + COLS)
        total = dot(wch[...], rc[:, at]) + dot(wcl[...], rc[:, at])
        fin[0, :, at] = total[:TOK].astype(BF)
        fin[1, :, at] = total[TOK:].astype(BF)
    mine = pl.ds(pl.multiple_of(c * H, H), H)
    done = send(fin.at[o], moe_hbm.at[:, mine], pair)
    copy = pltpu.make_async_copy(fin.at[c], moe_hbm.at[:, mine], out_sem.at[len(stores)])
    copy.start()
    stores.append(copy)
    gate_on(3)
    project(3)
    with phase("wait_done"):
        done.wait_recv()
    with phase("wait_stores"):
        for copy in stores:
            copy.wait()
    with phase("wait_sent"):
        for copy in sent:
            copy.wait_send()


def copies(z):
    return 6 + z.near + (z.near - 1) + z.stages + z.near * 4 + 3 * z.blocks + 4 + 2 * z.ep


def per_device(
    query, keys, values, gate_pre, log_decay, out_weight, expert_input, norm_gain, routes,
    route_weights, w_gate, w_up, w_down,
):
    rows, heads = query.shape[0], log_decay.shape[0]
    dk, dv = query.shape[1] // heads, values.shape[1] // heads
    tokens, width = expert_input.shape
    hidden, features = w_gate.shape[2], out_weight.shape[1]
    ep, tp = lax.axis_size("ep"), lax.axis_size("tp")
    z = Sizes(ep, tokens, width, routes.shape[1], rows, heads, dk, dv, hidden, features)
    inverse = (1.0 / 10000.0 ** np.linspace(0.0, 1.0, dk // 2)).astype(np.float32).astype(np.float64)
    inverse = np.tile(inverse, 128 // (dk // 2))
    spin = np.arange(BLOCK)[:, None] * inverse[None, :]
    base = (np.arange(ep * z.blocks) * BLOCK)[:, None] * inverse[None, :]
    spin = jnp.asarray(np.stack([np.cos(spin), np.sin(spin)]).astype(np.float32))
    base = jnp.asarray(np.stack([np.cos(base), np.sin(base)]).astype(np.float32))
    H, ONE, TWO, NEAR = z.half, z.one, z.two, z.near
    size = heads * dk
    depth = heads * dv
    inside = pl.BlockSpec(memory_space=VM)
    outside = pl.BlockSpec(memory_space=ANY)
    scratch = [
        VM((rows, size), BF), VM((rows, size), BF), VM((rows, depth), BF), VM((rows, depth), BF),
        VM((tp, depth, features), BF), VM((tokens, width), BF),
        VM((width, hidden), BF), VM((width, hidden), BF), VM((2, hidden, H), BF),
        VM((2, tokens, H), BF), VM((4, tokens, H), BF), VM((4, 8, tokens), F32),
        VM(((NEAR - 1) * TWO, H), BF), VM((NEAR * ONE, H), BF), VM((2, ep * TWO, H), BF),
        VM((ep * TWO, H), BF), VM((ep * TWO, H), BF), VM((ep * TWO, H), BF),
        VM((ep * ONE, H), BF), VM((ep * ONE, H), BF), VM((ep * ONE, H), BF), VM((2, tokens, H), BF),
        VM((2 * tokens, ep * ONE), BF), VM((2 * tokens, ep * ONE), BF),
        VM((NEAR * TWO, 4 * tokens), BF),
        VM((z.blocks, size, BLOCK), BF), VM((z.blocks, size, dv), F32),
        VM((z.blocks, heads, BLOCK), F32), VM((z.blocks, BLOCK, 8), F32),
        VM((z.stages, size + 16, dv), BF), VM((z.stages, size + 16, dv), BF), VM((size, dv), F32),
        VM((4, rows, depth), BF), VM((rows, features), BF),
        DMA((10,)), DMA((copies(z),)), DMA((copies(z),)), DMA((z.blocks + 1,)),
    ]
    return pl.pallas_call(
        functools.partial(kernel, z),
        in_specs=[outside] * 4 + [inside, outside, outside] + [inside] * 3 + [outside] * 3 + [inside] * 2,
        out_specs=[outside, outside],
        out_shape=[
            jax.ShapeDtypeStruct((rows, features), BF),
            jax.ShapeDtypeStruct((tokens, width), BF),
        ],
        scratch_shapes=scratch,
        compiler_params=pltpu.CompilerParams(
            collective_id=0, has_side_effects=True, vmem_limit_bytes=67043328
        ),
        cost_estimate=pl.CostEstimate(flops=10**10, bytes_accessed=20 << 20, transcendentals=0),
    )(
        query, keys, values, gate_pre, log_decay, out_weight.reshape(tp, depth, features), expert_input,
        norm_gain.reshape(1, width), routes.T, route_weights.T, w_gate, w_up, w_down, spin, base,
    )


def solution(mesh):
    placed = (
        P("ep", "tp"),
        P("ep", "tp"),
        P("ep", "tp"),
        P("ep", "tp"),
        P("tp", "ep"),
        P(None, "tp"),
        P(("ep", "tp"), None),
        P(),
        P(("ep", "tp"), None),
        P(("ep", "tp"), None),
        P("ep", None, "tp"),
        P("ep", None, "tp"),
        P("ep", "tp", None),
    )
    return jax.shard_map(
        per_device,
        mesh=mesh,
        in_specs=placed,
        out_specs=(P("ep", "tp"), P(("ep", "tp"), None)),
        check_vma=False,
    )
```

```python
import functools
import jax
import jax.numpy as jnp
import numpy as np
from jax import lax
from jax.experimental import pallas as pl
from jax.experimental.pallas import tpu as pltpu
from jax.sharding import PartitionSpec as P

BF = jnp.bfloat16
F32 = jnp.float32
VM = pltpu.VMEM
ANY = pl.ANY
MESH = pl.DeviceIdType.MESH
DMA = pltpu.SemaphoreType.DMA
BLOCK = 256
COLS = 512


def flip(index, bits):
    out = index
    bit = 1
    while bit <= bits:
        if bits & bit:
            out = out + bit - 2 * bit * lax.rem(lax.div(index, bit), 2)
        bit *= 2
    return out


phase = jax.named_scope


def dot(a, b):
    return jnp.dot(a, b, preferred_element_type=F32)


def turn(x, cos, sin, head_dim):
    width = x.shape[1]
    half = head_dim // 2
    lane = lax.broadcasted_iota(jnp.int32, x.shape, 1)
    first = lane % head_dim < half
    other = jnp.where(first, pltpu.roll(x, width - half, 1), pltpu.roll(x, half, 1))
    reps = width // cos.shape[1]
    return x * jnp.concatenate([cos] * reps, axis=1) + other * jnp.concatenate([sin] * reps, axis=1)


class Sizes:
    def __init__(self, ep, tokens, width, top, rows, heads, dk, dv, hidden, features):
        self.ep, self.tokens, self.width, self.top = ep, tokens, width, top
        self.rows, self.heads, self.dk, self.dv = rows, heads, dk, dv
        self.hidden, self.features = hidden, features
        self.half = width // 2
        self.cap = 3 * tokens * top // (2 * ep)
        self.one = -(-2 * self.cap // 16) * 16
        self.two = 2 * self.one
        self.near = ep // 2
        self.blocks = rows // BLOCK
        self.stages = ep.bit_length() - 1


def kernel(
    z,
    q_hbm, k_hbm, v_hbm, g_hbm, decay_ref, wo_hbm, tok_hbm, gain_ref, routes_ref, rweight_ref,
    wg_hbm, wu_hbm, wd_hbm, spin_ref, base_ref,
    mixed_hbm, moe_hbm,
    q_v, k_v, v_v, g_v, wo_v, tok_v, wg_v, wu_v, wd_v,
    nh, nb, meta, sn, sc, xf, yk, ys, yr, xr, zc, rc, fin,
    wch, wcl, pn, keyt, upd, run_v, runt_v, pack_s, pack_r, pre_v, gate_all, mix_v,
    load_sem, send_sem, recv_sem, out_sem,
):
    e = lax.axis_index("ep")
    t = lax.axis_index("tp")
    c = lax.rem(t, 2)
    o = 1 - c
    pair = (e, flip(t, 1))
    cross = (e, flip(t, 2))
    diag = (e, flip(t, 3))
    H, ONE, TWO, NEAR, TOK, CAP = z.half, z.one, z.two, z.near, z.tokens, z.cap
    used = [0]
    sent = []

    barrier = pltpu.get_barrier_semaphore()
    peers = [(flip(e, d), t) for d in range(1, z.ep)] + [pair, cross, diag]
    for peer in peers:
        pl.semaphore_signal(barrier, inc=1, device_id=peer, device_id_type=MESH)

    loads = {}

    def load(name, src, dst):
        copy = pltpu.make_async_copy(src, dst, load_sem.at[len(loads)])
        copy.start()
        loads[name] = copy

    load("tok", tok_hbm, tok_v)
    load("k", k_hbm, k_v)
    load("v", v_hbm, v_v)
    load("q", q_hbm, q_v)
    load("g", g_hbm, g_v)
    load("wg", wg_hbm.at[0], wg_v)
    load("wu", wu_hbm.at[0], wu_v)
    for h in range(2):
        load("wd%d" % h, wd_hbm.at[0, :, pl.ds(h * H, H)], wd_v.at[h])
    load("wo", wo_hbm, wo_v)

    def prepare(src, dst, device):
        i = used[0]
        used[0] += 1
        copy = pltpu.make_async_remote_copy(
            src_ref=src, dst_ref=dst, send_sem=send_sem.at[i], recv_sem=recv_sem.at[i],
            device_id=device, device_id_type=MESH,
        )
        sent.append(copy)
        return copy

    def send(src, dst, device):
        copy = prepare(src, dst, device)
        copy.start()
        return copy

    both = jnp.concatenate([routes_ref[...].astype(F32), rweight_ref[...]], axis=0)
    meta[c] = jnp.concatenate([both] * (8 // both.shape[0]), axis=0)

    with phase("wait_tok"):
        loads["tok"].wait()
    x = tok_v[...].astype(F32)
    centered = x - jnp.mean(x, axis=-1, keepdims=True)
    variance = jnp.mean(centered * centered, axis=-1, keepdims=True)
    normed = (centered * lax.rsqrt(variance + 1e-05) * gain_ref[...]).astype(BF)
    nh[0] = normed[:, :H]
    nh[1] = normed[:, H:]
    heads, dk, dv = z.heads, z.dk, z.dv
    size = heads * dk
    run = decay_ref[...]
    along = lax.broadcasted_iota(jnp.int32, run.shape, 1) % BLOCK
    step = 1
    while step < BLOCK:
        run = run + jnp.where(along >= step, pltpu.roll(run, step, 1), 0.0)
        step *= 2
    for b in range(z.blocks):
        part = run[:, b * BLOCK : (b + 1) * BLOCK]
        run_v[b] = part
        runt_v[b] = jnp.concatenate([part] * (8 // heads), axis=0).T

    def tables(b):
        at = e * z.blocks + b
        cos_b = base_ref[0, pl.ds(at, 1), :]
        sin_b = base_ref[1, pl.ds(at, 1), :]
        cos = cos_b * spin_ref[0] - sin_b * spin_ref[1]
        sin = sin_b * spin_ref[0] + cos_b * spin_ref[1]
        lane = lax.broadcasted_iota(jnp.int32, sin.shape, 1)
        return cos, jnp.where(lane % dk < dk // 2, -sin, sin)

    loads["k"].wait()
    loads["v"].wait()
    state = [jnp.zeros((dk, dv), F32)] * heads
    total = [jnp.zeros((1, 1), F32)] * heads
    for b in range(z.blocks):
        at = slice(b * BLOCK, (b + 1) * BLOCK)
        cos, sin = tables(b)
        kt = (turn(k_v[at, :].astype(F32), cos, sin, dk) * dk ** (-0.5)).T
        keyt[b] = kt.astype(BF)
        for h in range(heads):
            rows = slice(h * dk, (h + 1) * dk)
            run_row = run_v[b, h : h + 1, :]
            closing = run_row[:, BLOCK - 1 : BLOCK]
            scaled = (kt[rows, :] * jnp.exp(closing - run_row)).astype(BF)
            new = dot(scaled, v_v[at, h * dv : (h + 1) * dv])
            upd[b, rows, :] = new
            state[h] = state[h] * jnp.exp(closing) + new
            total[h] = total[h] + closing
    group = jnp.concatenate(state, axis=0)
    fade = [jnp.broadcast_to(jnp.exp(x), (1, dv)) for x in total]
    prefix = jnp.zeros((size, dv), F32)
    prefade = jnp.ones((size, dv), F32)
    scans = []

    def spread(fade):
        return jnp.concatenate([jnp.broadcast_to(x, (dk, dv)) for x in fade], axis=0)

    @phase("scan_send")
    def scan_send(s):
        pack_s[s, 0:size] = group.astype(BF)
        pack_s[s, size:] = jnp.concatenate(fade * (16 // heads), axis=0).astype(BF)
        scans.append(send(pack_s.at[s], pack_r.at[s], (flip(e, 1 << s), t)))

    @phase("scan_recv")
    def scan_recv(s, group, fade, prefix, prefade):
        scans[s].wait_recv()
        other = pack_r[s, 0:size].astype(F32)
        rows = pack_r[s, size:].astype(F32)
        other_fade = [rows[h : h + 1] for h in range(heads)]
        all_fade = spread(other_fade)
        later = lax.rem(lax.div(e, 1 << s), 2) == 1
        prefix = jnp.where(later, prefix + prefade * other, prefix)
        prefade = jnp.where(later, prefade * all_fade, prefade)
        group = jnp.where(later, other * spread(fade) + group, group * all_fade + other)
        return group, [a * b for a, b in zip(fade, other_fade)], prefix, prefade

    with phase("barrier"):
        pl.semaphore_wait(barrier, len(peers))
    metas = [
        send(meta.at[c], meta.at[c], pair),
        send(meta.at[c], meta.at[2 + c], cross),
        send(meta.at[c], meta.at[2 + c], diag),
    ]
    toks = [
        send(nh.at[o], nb.at[c], pair),
        send(nh.at[c], nb.at[2 + c], cross),
        send(nh.at[o], nb.at[2 + c], diag),
    ]
    scan_send(0)
    nb[c] = nh[c]


    with phase("wait_metas"):
        for copy in metas:
            copy.wait_recv()
    every = 4 * TOK
    info = jnp.concatenate([meta[g].T for g in range(4)], axis=0)
    number = lax.broadcasted_iota(jnp.int32, (every, 128), 1)
    token = lax.broadcasted_iota(jnp.int32, (every, 1), 0)
    away = lax.div(token, 2 * TOK)
    side = lax.rem(lax.div(token, TOK), 2)
    rel = [jnp.bitwise_xor(info[:, r : r + 1].astype(jnp.int32), e) for r in range(2)]
    hits = [(rel[r] == number).astype(F32) for r in range(2)]
    i = lax.broadcasted_iota(jnp.int32, (every, every), 0)
    j = lax.broadcasted_iota(jnp.int32, (every, every), 1)
    earlier = ((j < i) & (lax.div(i, TOK) == lax.div(j, TOK))).astype(F32).astype(BF)
    before = dot(earlier, (hits[0] + hits[1]).astype(BF))
    near_lane = lax.broadcasted_iota(jnp.int32, (every, NEAR * TWO), 1)
    far_lane = lax.broadcasted_iota(jnp.int32, (2 * TOK, NEAR * ONE), 1)
    near_place = jnp.zeros((every, NEAR * TWO), F32)
    far_place = jnp.zeros((2 * TOK, NEAR * ONE), F32)
    all_lane = lax.broadcasted_iota(jnp.int32, (2 * TOK, z.ep * ONE), 1)
    all_weight = jnp.zeros((2 * TOK, z.ep * ONE), F32)
    for r in range(2):
        slot = jnp.sum(before * hits[r], axis=1, keepdims=True).astype(jnp.int32) + side * CAP
        weight = info[: 2 * TOK, 2 + r : 3 + r]
        near_at = jnp.where(rel[r] < NEAR, rel[r] * TWO + away * ONE + slot, -1)
        far_at = jnp.where(rel[r] >= NEAR, (rel[r] - NEAR) * ONE + slot, -1)[: 2 * TOK]
        near_here = near_at == near_lane
        far_here = far_at == far_lane
        near_place = near_place + jnp.where(near_here, 1.0, 0.0)
        all_at = (rel[r] * ONE + slot)[: 2 * TOK]
        all_weight = all_weight + jnp.where(all_at == all_lane, weight, 0.0)
        far_place = far_place + jnp.where(far_here, 1.0, 0.0)
    top = all_weight.astype(BF)
    wch[...] = top
    wcl[...] = (all_weight - top.astype(F32)).astype(BF)
    pn[...] = near_place.T.astype(BF)
    placing = far_place.T.astype(BF)

    with phase("wait_pair_tok"):
        toks[0].wait_recv()
    for col in range(0, H, COLS):
        rows = jnp.concatenate([nb[g, :, col : col + COLS] for g in range(2)], axis=0)
        sc[:, col : col + COLS] = dot(placing, rows).astype(BF)
    far_in = [
        prepare(sc.at[pl.ds(d * ONE, ONE)], xf.at[c, pl.ds((NEAR + d) * TWO, ONE)], (flip(e, NEAR + d), t))
        for d in range(NEAR)
    ]

    def far_send(d):
        far_in[d].start()

    quarter = z.ep // 4
    first = list(range(quarter))
    second = list(range(quarter, NEAR))
    cut = max(1, quarter // 2)
    outer = lax.rem(lax.div(e, NEAR), 2) == lax.rem(lax.div(e, max(1, NEAR // 2)), 2)

    @pl.when(jnp.logical_not(outer))
    def _():
        for d in second[:cut]:
            far_send(d)

    for s in range(1, z.stages):
        group, fade, prefix, prefade = scan_recv(s - 1, group, fade, prefix, prefade)
        scan_send(s)

    pairs = {}

    def to_pair(at, count):
        where = xf.at[c, pl.ds(at, count)]
        pairs[at] = send(where, where, pair)

    far_x = {}

    @phase("relay")
    def relay(d):
        far_in[d].wait_recv()
        at = (NEAR + d) * TWO
        far_x[d] = send(xf.at[c, pl.ds(at, ONE)], xf.at[c, pl.ds(at + ONE, ONE)], cross)
        to_pair(at, ONE)

    @phase("relay_on")
    def relay_on(d):
        far_x[d].wait_recv()
        to_pair((NEAR + d) * TWO + ONE, ONE)

    @phase("relay_near")
    def relay_near(d):
        near_in[d].wait_recv()
        to_pair(d * TWO, TWO)

    near_gate, far_gate = [], []
    pieces = [(b * BLOCK, BLOCK) for b in range(z.blocks - 1)]
    pieces += [(z.rows - BLOCK + h * (BLOCK // 2), BLOCK // 2) for h in range(2)]

    @phase("mix")
    def mix(b, state):
        at = slice(b * BLOCK, (b + 1) * BLOCK)
        cos, sin = tables(b)
        q = turn(q_v[at, :].astype(F32), cos, sin, dk)
        row = lax.broadcasted_iota(jnp.int32, (BLOCK, BLOCK), 0)
        col = lax.broadcasted_iota(jnp.int32, (BLOCK, BLOCK), 1)
        causal = row >= col
        after = []
        for h in range(heads):
            rows = slice(h * dk, (h + 1) * dk)
            run_row = run_v[b, h : h + 1, :]
            run_col = runt_v[b, :, h : h + 1]
            closing = run_row[:, BLOCK - 1 : BLOCK]
            qh = q[:, rows]
            vh = v_v[at, h * dv : (h + 1) * dv]
            weights = jnp.where(causal, jnp.exp(jnp.where(causal, run_col - run_row, 0.0)), 0.0)
            scores = dot(qh.astype(BF), keyt[b, rows, :]) * weights
            out = dot(scores.astype(BF), vh)
            carried = state[rows, :]
            out = out + dot((qh * jnp.exp(run_col)).astype(BF), carried.astype(BF))
            after.append(carried * jnp.exp(closing) + upd[b, rows, :])
            centered = out - jnp.mean(out, axis=-1, keepdims=True)
            variance = jnp.mean(centered * centered, axis=-1, keepdims=True)
            gate = g_v[at, h * dv : (h + 1) * dv].astype(F32)
            act = gate / (1.0 + jnp.exp(-gate))
            gate_all[0, at, h * dv : (h + 1) * dv] = (act * (centered * lax.rsqrt(variance + 1e-06))).astype(BF)
        return jnp.concatenate(after, axis=0)

    @phase("gate_x")
    def gate_x(b):
        gate_ready(b)
        gate_start(b)

    def gate_ready(b):
        at = pl.ds(*pieces[b])
        far_gate.append(prepare(gate_all.at[0, at], gate_all.at[2, at], cross))
        near_gate.append(prepare(gate_all.at[0, at], gate_all.at[1, at], pair))

    def gate_start(b):
        far_gate[b].start()
        near_gate[b].start()

    last_gate = []

    @phase("gate_on")
    def gate_on(b):
        far_gate[b].wait_recv()
        at = pl.ds(*pieces[b])
        last_gate.append(send(gate_all.at[2, at], gate_all.at[3, at], pair))

    stores = []

    @phase("project")
    def project(b):
        near_gate[b].wait_recv()
        last_gate[b].wait_recv()
        at = pl.ds(*pieces[b])
        sum_ = dot(gate_all[0, at], wo_v[t])
        for g in range(1, 4):
            sum_ = sum_ + dot(gate_all[g, at], wo_v[flip(t, g)])
        mix_v[at, :] = sum_.astype(BF)
        copy = pltpu.make_async_copy(mix_v.at[at], mixed_hbm.at[at], out_sem.at[len(stores)])
        copy.start()
        stores.append(copy)

    trade = {}

    @phase("ffn")
    def ffn(part):
        at = part * quarter * TWO
        count = quarter * TWO
        rows = slice(at, at + count)
        gate = dot(xf[0, rows], wg_v[0:H]) + dot(xf[1, rows], wg_v[H:])
        up = dot(xf[0, rows], wu_v[0:H]) + dot(xf[1, rows], wu_v[H:])
        hidden = (gate * up / (1.0 + jnp.exp(-gate))).astype(BF)
        ys[rows] = dot(hidden, wd_v[o]).astype(BF)
        where = pl.ds(at, count)
        trade[part] = send(ys.at[where], yr.at[where], pair)
        yk[rows] = dot(hidden, wd_v[c]).astype(BF)

    @phase("wait_pairs")
    def wait_pairs(part):
        for d in range(part * quarter, (part + 1) * quarter):
            pairs[d * TWO].wait_recv()
            if d >= NEAR:
                pairs[d * TWO + ONE].wait_recv()

    @phase("core_sum")
    def core_sum(part):
        trade[part].wait_recv()
        at = part * quarter * TWO
        rows = slice(at, at + quarter * TWO)
        yk[rows] = (yk[rows].astype(F32) + yr[rows].astype(F32)).astype(BF)

    cross_sum, home_out = {}, {}

    def back(part):
        core_sum(part)
        push(part)

    @phase("back")
    def push(part):
        for d in range(part * quarter, (part + 1) * quarter):
            cross_sum[d] = send(yk.at[pl.ds(d * TWO + ONE, ONE)], xr.at[pl.ds(d * ONE, ONE)], cross)

    @phase("home")
    def home(part):
        for d in range(part * quarter, (part + 1) * quarter):
            cross_sum[d].wait_recv()
            rows = slice(d * ONE, (d + 1) * ONE)
            full = (yk[d * TWO : d * TWO + ONE].astype(F32) + xr[rows].astype(F32)).astype(BF)
            if d == 0:
                rc[rows] = full
            else:
                zc[rows] = full
                home_out[d] = send(zc.at[pl.ds(d * ONE, ONE)], rc.at[pl.ds(d * ONE, ONE)], (flip(e, d), t))

    group, fade, prefix, prefade = scan_recv(z.stages - 1, group, fade, prefix, prefade)
    for d in first:
        far_send(d)
    with phase("wait_qg"):
        loads["q"].wait()
        loads["g"].wait()
    state = mix(0, prefix)
    gate_x(0)

    with phase("wait_x_tok"):
        toks[1].wait_recv()
        toks[2].wait_recv()
    for col in range(0, H, COLS):
        rows = jnp.concatenate([nb[g, :, col : col + COLS] for g in range(4)], axis=0)
        made = dot(pn[...], rows).astype(BF)
        xf[c, 0:TWO, col : col + COLS] = made[0:TWO]
        sn[:, col : col + COLS] = made[TWO:]
    near_in = {}
    for d in range(1, NEAR):
        near_in[d] = send(sn.at[pl.ds((d - 1) * TWO, TWO)], xf.at[c, pl.ds(d * TWO, TWO)], (flip(e, d), t))
        if d == NEAR - 2:

            @pl.when(outer)
            def _():
                for i in second[:cut]:
                    far_send(i)

            for i in second[cut:]:
                far_send(i)
    to_pair(0, TWO)

    state = mix(1, state)
    gate_ready(1)

    @pl.when(outer)
    def _():
        gate_start(1)

    state = mix(2, state)
    for d in first[:cut]:
        relay(d)
    mix(3, state)
    with phase("wait_w"):
        for name in ("wg", "wu", "wd0", "wd1"):
            loads[name].wait()
    for d in first[cut:]:
        relay(d)

    @pl.when(jnp.logical_not(outer))
    def _():
        gate_start(1)

    gate_x(2)
    for d in first:
        relay_on(d)
    wait_pairs(2)
    ffn(2)
    for d in range(1, quarter):
        relay_near(d)
    back(2)
    wait_pairs(0)
    ffn(0)
    for d in second:
        relay(d)
    for d in range(quarter, NEAR):
        relay_near(d)
    wait_pairs(1)
    ffn(1)
    home(2)
    for d in second:
        relay_on(d)
    back(1)
    wait_pairs(3)
    ffn(3)
    core_sum(0)
    back(3)
    push(0)
    gate_x(3)
    gate_x(4)
    with phase("wait_wo"):
        loads["wo"].wait()
    for b in range(3):
        gate_on(b)
    home(1)
    project(0)
    home(3)
    project(1)
    home(0)
    project(2)

    with phase("wait_home"):
        for d in range(1, z.ep):
            home_out[d].wait_recv()
    for col in range(0, H, COLS):
        at = slice(col, col + COLS)
        total = dot(wch[...], rc[:, at]) + dot(wcl[...], rc[:, at])
        fin[0, :, at] = total[:TOK].astype(BF)
        fin[1, :, at] = total[TOK:].astype(BF)
    mine = pl.ds(pl.multiple_of(c * H, H), H)
    done = send(fin.at[o], moe_hbm.at[:, mine], pair)
    copy = pltpu.make_async_copy(fin.at[c], moe_hbm.at[:, mine], out_sem.at[len(stores)])
    copy.start()
    stores.append(copy)
    for b in (3, 4):
        gate_on(b)
    for b in (3, 4):
        project(b)
    with phase("wait_done"):
        done.wait_recv()
    with phase("wait_stores"):
        for copy in stores:
            copy.wait()
    with phase("wait_sent"):
        for copy in sent:
            copy.wait_send()


def copies(z):
    return 6 + z.near + (z.near - 1) + z.stages + z.near * 4 + 3 * (z.blocks + 1) + 4 + 2 * z.ep


def per_device(
    query, keys, values, gate_pre, log_decay, out_weight, expert_input, norm_gain, routes,
    route_weights, w_gate, w_up, w_down,
):
    rows, heads = query.shape[0], log_decay.shape[0]
    dk, dv = query.shape[1] // heads, values.shape[1] // heads
    tokens, width = expert_input.shape
    hidden, features = w_gate.shape[2], out_weight.shape[1]
    ep, tp = lax.axis_size("ep"), lax.axis_size("tp")
    z = Sizes(ep, tokens, width, routes.shape[1], rows, heads, dk, dv, hidden, features)
    inverse = (1.0 / 10000.0 ** np.linspace(0.0, 1.0, dk // 2)).astype(np.float32).astype(np.float64)
    inverse = np.tile(inverse, 128 // (dk // 2))
    spin = np.arange(BLOCK)[:, None] * inverse[None, :]
    base = (np.arange(ep * z.blocks) * BLOCK)[:, None] * inverse[None, :]
    spin = jnp.asarray(np.stack([np.cos(spin), np.sin(spin)]).astype(np.float32))
    base = jnp.asarray(np.stack([np.cos(base), np.sin(base)]).astype(np.float32))
    H, ONE, TWO, NEAR = z.half, z.one, z.two, z.near
    size = heads * dk
    depth = heads * dv
    inside = pl.BlockSpec(memory_space=VM)
    outside = pl.BlockSpec(memory_space=ANY)
    scratch = [
        VM((rows, size), BF), VM((rows, size), BF), VM((rows, depth), BF), VM((rows, depth), BF),
        VM((tp, depth, features), BF), VM((tokens, width), BF),
        VM((width, hidden), BF), VM((width, hidden), BF), VM((2, hidden, H), BF),
        VM((2, tokens, H), BF), VM((4, tokens, H), BF), VM((4, 8, tokens), F32),
        VM(((NEAR - 1) * TWO, H), BF), VM((NEAR * ONE, H), BF), VM((2, ep * TWO, H), BF),
        VM((ep * TWO, H), BF), VM((ep * TWO, H), BF), VM((ep * TWO, H), BF),
        VM((ep * ONE, H), BF), VM((ep * ONE, H), BF), VM((ep * ONE, H), BF), VM((2, tokens, H), BF),
        VM((2 * tokens, ep * ONE), BF), VM((2 * tokens, ep * ONE), BF),
        VM((NEAR * TWO, 4 * tokens), BF),
        VM((z.blocks, size, BLOCK), BF), VM((z.blocks, size, dv), F32),
        VM((z.blocks, heads, BLOCK), F32), VM((z.blocks, BLOCK, 8), F32),
        VM((z.stages, size + 16, dv), BF), VM((z.stages, size + 16, dv), BF), VM((size, dv), F32),
        VM((4, rows, depth), BF), VM((rows, features), BF),
        DMA((10,)), DMA((copies(z),)), DMA((copies(z),)), DMA((z.blocks + 2,)),
    ]
    return pl.pallas_call(
        functools.partial(kernel, z),
        in_specs=[outside] * 4 + [inside, outside, outside] + [inside] * 3 + [outside] * 3 + [inside] * 2,
        out_specs=[outside, outside],
        out_shape=[
            jax.ShapeDtypeStruct((rows, features), BF),
            jax.ShapeDtypeStruct((tokens, width), BF),
        ],
        scratch_shapes=scratch,
        compiler_params=pltpu.CompilerParams(
            collective_id=0, has_side_effects=True, vmem_limit_bytes=67043328
        ),
        cost_estimate=pl.CostEstimate(flops=10**10, bytes_accessed=20 << 20, transcendentals=0),
    )(
        query, keys, values, gate_pre, log_decay, out_weight.reshape(tp, depth, features), expert_input,
        norm_gain.reshape(1, width), routes.T, route_weights.T, w_gate, w_up, w_down, spin, base,
    )


def solution(mesh):
    placed = (
        P("ep", "tp"),
        P("ep", "tp"),
        P("ep", "tp"),
        P("ep", "tp"),
        P("tp", "ep"),
        P(None, "tp"),
        P(("ep", "tp"), None),
        P(),
        P(("ep", "tp"), None),
        P(("ep", "tp"), None),
        P("ep", None, "tp"),
        P("ep", None, "tp"),
        P("ep", "tp", None),
    )
    return jax.shard_map(
        per_device,
        mesh=mesh,
        in_specs=placed,
        out_specs=(P("ep", "tp"), P(("ep", "tp"), None)),
        check_vma=False,
    )
```
